256 devices in a mesh: grp: 2 (over y), sp: 16 (over z), tp: 8 (over x, core).
Axes of the slice: x: 4, y: 2, z: 16, core: 2. Of those that a mesh axis runs over, the one named last changes fastest.
The devices are a block of a 4x16x16 slice.
Arguments:
- queries: bfloat16 [16384, 2048], P(('grp', 'sp'), 'tp'), parts along dimension 0, may hold values from -6 to 6
- key_vectors: bfloat16 [16384, 2048], P(('grp', 'sp'), 'tp'), parts along dimension 0, may hold values from -6 to 6
- value_vectors: bfloat16 [16384, 2048], P(('grp', 'sp'), 'tp'), parts along dimension 0, may hold values from -6 to 6
- forget_sums: float32 [16384, 16], P(('grp', 'sp'), 'tp'), parts along dimension 0, may hold values from -8192 to 0, as said below
- residual: bfloat16 [16384, 2048], P(('grp', 'sp'), 'tp'), parts along dimension 0, may hold values from -20 to 20
- query_gain: float32 [128], replicated, may hold values from 0.5 to 5
- key_gain: float32 [128], replicated, may hold values from 0.5 to 5
- out_weight: bfloat16 [2048, 2048], P(None, 'tp'), may hold values from -0.125 to 0.125
- norm_gain: float32 [2048], replicated, may hold values from 0.1 to 1.9
- gate_weight: bfloat16 [2048, 5504], P('sp', 'tp'), may hold values from -0.125 to 0.125
- up_weight: bfloat16 [2048, 5504], P('sp', 'tp'), may hold values from -0.125 to 0.125
- down_weight: bfloat16 [2048, 5504], P('sp', 'tp'), may hold values from -0.078125 to 0.078125
Outputs:
- layer_output: bfloat16 [16384, 2048], P(('grp', 'sp'), 'tp'), parts along dimension 0
The draws below stay inside these ranges and needn't reach their ends.
There are 2 independent parts, one for each index of `grp`. The reference program is written for one: setup_inputs(seed, part) draws one part's arguments, and reference() takes and returns one part's arrays. A program takes and returns all parts, laid end to end along the dimension named above; an argument that names none is the same for every part. Nothing has to cross between parts.
Inputs may be any that keep to these rules, and one draw needn't show every extreme that they name: `forget_sums`: along positions each head's values never rise.
All inputs are finite; a program needn't handle non-finite values.
Results may differ from the reference program's by a relative error of at most 0.011.
Values may be sent and summed in bfloat16 or wider, within the bound.
No kernel may reach another device: no remote copies, remote signals or barrier semaphores. Data moves between devices by JAX's collectives and lax.ppermute only.
A program may use at most 128 MiB of HBM per device.

```python
import math
import jax
import jax.numpy as jnp
from jax import lax

D = 2048
HEADS = 16
HEAD = 128
FF = 5504
TOK_DEV = 512
TOKENS = 8192
N_TP = 8


def paired_rows(key):
    base = jax.random.fold_in(key, 101)
    first, second = jax.random.split(base, 2)
    width = HEADS * HEAD
    query_rows = jax.random.normal(first, (TOKENS, width), jnp.float32)
    key_rows = jax.random.normal(second, (TOKENS, width), jnp.float32)
    return (jnp.clip(query_rows, -6.0, 6.0), jnp.clip(key_rows, -6.0, 6.0))


def draw_queries(key, part):
    return paired_rows(key)[0].astype(jnp.bfloat16)


def draw_key_vectors(key, part):
    return paired_rows(key)[1].astype(jnp.bfloat16)


def draw_gain_common(key, salt):
    inner = jax.random.fold_in(key, salt)
    return jnp.exp(jax.random.uniform(inner, (HEAD,), jnp.float32, math.log(0.5), math.log(2.0)))


def draw_query_gain(key, part):
    return draw_gain_common(key, 201)


def draw_key_gain(key, part):
    return draw_gain_common(key, 202)


def draw_forget_sums(key, part):
    base = jax.random.fold_in(key, 301)
    parts = jax.random.split(base, 7)
    order = jax.random.permutation(parts[0], HEADS)
    fast = order < HEADS // 2
    fast_rate = jnp.exp(jax.random.uniform(parts[1], (HEADS,), jnp.float32, math.log(1.0 / 80.0), math.log(1.0 / 30.0)))
    slow_rate = jnp.exp(jax.random.uniform(parts[2], (HEADS,), jnp.float32, math.log(0.5), math.log(2.0))) * (0.4 / TOKENS)
    rate = jnp.where(fast, fast_rate, slow_rate)
    noise = jnp.exp(jax.random.uniform(parts[3], (TOKENS, HEADS), jnp.float32, math.log(0.5), math.log(2.0)))
    block_factor = jnp.exp(jax.random.uniform(parts[4], (TOKENS // TOK_DEV,), jnp.float32, math.log(0.5), math.log(2.0)))
    block_factor = jnp.repeat(block_factor, TOK_DEV)
    log_gates = -rate[None, :] * noise * block_factor[:, None]
    places = jax.random.randint(parts[5], (3,), 0, TOKENS)
    drops = jnp.log(jax.random.uniform(parts[6], (3, HEADS), jnp.float32, 0.5, 0.8))
    marks = (jnp.arange(TOKENS)[:, None] == places[None, :]).astype(jnp.float32)
    log_gates = log_gates + jnp.dot(marks, drops)
    return jnp.cumsum(log_gates, axis=0)


def draw_residual(key, part):
    base = jax.random.fold_in(key, 401)
    parts = jax.random.split(base, 3)
    column_scale = jnp.exp(jnp.linspace(math.log(0.4), math.log(3.0), D)) * jnp.exp(jax.random.uniform(parts[0], (D,), jnp.float32, math.log(0.7), math.log(1.4)))
    rows = jnp.clip(jax.random.normal(parts[2], (TOKENS, D), jnp.float32), -5.0, 5.0)
    return jnp.clip(rows * column_scale[None, :], -20.0, 20.0).astype(jnp.bfloat16)


def level_of(stream_key, dims, pieces, smallest, top_value):
    def one(axis_at, shards_of):
        draws = jax.random.uniform(jax.random.fold_in(jax.random.fold_in(stream_key, 6), axis_at), (shards_of,), jnp.float32, smallest / len(pieces), top_value / len(pieces))
        return jnp.repeat(jnp.exp(draws), dims[axis_at] // shards_of).reshape((-1,) + (1,) * (len(dims) - axis_at - 1))

    level = one(*pieces[0])
    for cut in pieces[1:]:
        level = level * one(*cut)
    return level


def scatter_about(rng, extent, deviation, limit, shards=(), kind=jnp.bfloat16):
    level = level_of(rng, extent, shards, -0.22, 0.18) if shards else 1.0
    drawn = jax.random.normal(rng, extent, jnp.float32) * deviation * level
    return jnp.minimum(jnp.maximum(drawn, -limit), limit).astype(kind)


def setup_inputs(seed: int = 0, part: int = 0) -> dict:
    key_of = jax.random.split(jax.random.key(seed), 13)
    own_keys = jax.random.split(jax.random.fold_in(key_of[12], part), 13)
    queries = draw_queries(jax.random.fold_in(jax.random.fold_in(key_of[12], part), 71), part)
    key_vectors = draw_key_vectors(jax.random.fold_in(jax.random.fold_in(key_of[12], part), 71), part)
    value_vectors = scatter_about(own_keys[2], (TOKENS, HEADS * HEAD), 1.0, 6.0, ((0, 16), (1, 8)))
    forget_sums = draw_forget_sums(jax.random.fold_in(jax.random.fold_in(key_of[12], part), 71), part)
    residual = draw_residual(jax.random.fold_in(jax.random.fold_in(key_of[12], part), 71), part)
    query_gain = draw_query_gain(jax.random.fold_in(key_of[12], 71), part)
    key_gain = draw_key_gain(jax.random.fold_in(key_of[12], 71), part)
    out_weight = scatter_about(key_of[7], (HEADS * HEAD, D), (HEADS * HEAD) ** -0.5, 0.125, ((1, 8),))
    norm_gain = jnp.clip(1.0 + 0.18 * jax.random.normal(key_of[8], (D,), jnp.float32), 0.1, 1.9)
    gate_weight = scatter_about(key_of[9], (D, FF), D ** -0.5, 0.125, ((0, 16), (1, 8)))
    up_weight = scatter_about(key_of[10], (D, FF), D ** -0.5, 0.125, ((0, 16), (1, 8)))
    down_weight = scatter_about(key_of[11], (D, FF), FF ** -0.5, 0.078125, ((0, 16), (1, 8)))
    return {"queries": queries, "key_vectors": key_vectors, "value_vectors": value_vectors, "forget_sums": forget_sums, "residual": residual, "query_gain": query_gain, "key_gain": key_gain, "out_weight": out_weight, "norm_gain": norm_gain, "gate_weight": gate_weight, "up_weight": up_weight, "down_weight": down_weight}


eps = 1e-06

def head_norm(rows_in, gain):
    count = rows_in.shape[0]
    split = rows_in.reshape(count, -1, HEAD).astype(jnp.float32)
    factor = lax.rsqrt(lax.optimization_barrier(jnp.mean(split * split, axis=2, keepdims=True)) + eps)
    return (split * factor * gain).astype(jnp.bfloat16)

def reference(queries, key_vectors, value_vectors, forget_sums, residual, query_gain, key_gain, out_weight, norm_gain, gate_weight, up_weight, down_weight):
    query_norm = head_norm(queries, query_gain)
    key_norm = lax.optimization_barrier(head_norm(key_vectors, key_gain)).astype(jnp.float32)
    values = value_vectors.reshape(TOKENS, HEADS, HEAD).astype(jnp.float32)
    biases = forget_sums.T
    block = math.gcd(TOKENS, 512)
    key_pos = jnp.arange(TOKENS, dtype=jnp.int32)
    factor = 1.0 / math.sqrt(HEAD)

    def attend(index):
        first = index * block
        query_block = lax.optimization_barrier(lax.dynamic_slice_in_dim(query_norm, first, block, 0)).astype(jnp.float32)
        scores = jnp.einsum('qhd,khd->hqk', query_block, key_norm) * factor
        query_bias = lax.dynamic_slice_in_dim(biases, first, block, 1)
        scores = scores + query_bias[:, :, None] - biases[:, None, :]
        query_pos = first + jnp.arange(block, dtype=jnp.int32)
        allowed = key_pos[None, :] <= query_pos[:, None]
        scores = jnp.where(allowed[None], scores, -jnp.inf)
        top = lax.optimization_barrier(jnp.max(scores, axis=2, keepdims=True))
        raised = jnp.exp(scores - top)
        totals = lax.optimization_barrier(jnp.sum(raised, axis=2))
        weights = lax.optimization_barrier(raised.astype(jnp.bfloat16)).astype(jnp.float32)
        summed = jnp.einsum('hqk,khd->qhd', weights, values)
        return (summed / totals.T[:, :, None]).astype(jnp.bfloat16)
    attended = lax.map(attend, jnp.arange(TOKENS // block, dtype=jnp.int32)).reshape(TOKENS, HEADS * HEAD)
    projected = jnp.dot(attended, out_weight, preferred_element_type=jnp.float32)
    middle = (residual.astype(jnp.float32) + projected).astype(jnp.bfloat16)
    whole = middle.astype(jnp.float32)
    normed = (whole * lax.rsqrt(lax.optimization_barrier(jnp.mean(whole * whole, axis=1, keepdims=True)) + eps) * norm_gain).astype(jnp.bfloat16)
    gate = jnp.dot(normed, gate_weight, preferred_element_type=jnp.float32)
    upward = jnp.dot(normed, up_weight, preferred_element_type=jnp.float32)
    hidden = (jax.nn.silu(gate) * upward).astype(jnp.bfloat16)
    width = FF // N_TP

    def add_block(index, total):
        start = (index * width).astype(jnp.int32)
        hidden_part = lax.dynamic_slice_in_dim(hidden, start, width, 1)
        weight_part = lax.dynamic_slice_in_dim(down_weight, start, width, 1)
        partial_value = lax.dot_general(hidden_part, weight_part, (((1,), (1,)), ((), ())), preferred_element_type=jnp.float32)
        rounded = lax.optimization_barrier(partial_value.astype(jnp.bfloat16))
        return total + rounded.astype(jnp.float32)
    down = lax.fori_loop(0, N_TP, add_block, jnp.zeros((TOKENS, D), jnp.float32))
    return (whole + down).astype(jnp.bfloat16)
```

```python
import functools
import math

import jax
import jax.numpy as jnp
from jax import lax
from jax.experimental import pallas as pl
from jax.experimental.pallas import tpu as pltpu
from jax.sharding import PartitionSpec as P


HEAD = 128
EPS = 1e-06
LOG2E = math.log2(math.e)
SCALE = LOG2E / math.sqrt(HEAD)
BF = jnp.bfloat16
F32 = jnp.float32
EXTRA = 16
VMEM = pl.BlockSpec(memory_space=pltpu.VMEM)
SMEM = pl.BlockSpec(memory_space=pltpu.SMEM)
MIB = 1024 * 1024


def call(kernel, out_shape, specs, name, limit, scratch=()):
    return pl.pallas_call(
        kernel,
        out_shape=out_shape,
        in_specs=specs,
        out_specs=jax.tree.map(lambda _: VMEM, out_shape),
        scratch_shapes=list(scratch),
        compiler_params=pltpu.CompilerParams(vmem_limit_bytes=limit * MIB),
        name=name,
    )


def turn(x, axis, size, by):
    return lax.ppermute(x, axis, [(i, (i + by) % size) for i in range(size)])


def swap_core(x, size):
    return lax.ppermute(x, "tp", [(i, i ^ 1) for i in range(size)])


def turn_x(x, size, by):
    return lax.ppermute(x, "tp", [(i, (i + 2 * by) % size) for i in range(size)])


def swap_pair(x, size):
    return lax.ppermute(x, "grp", [(i, i ^ 1) for i in range(size)])


def prep_kernel(q_ref, k_ref, v_ref, qg_ref, kg_ref, f_ref, qo_ref, kv_ref):
    rows = q_ref.shape[0]
    for h in range(q_ref.shape[1] // HEAD):
        cols = slice(h * HEAD, (h + 1) * HEAD)
        for ref, gain, out, scale in ((k_ref, kg_ref, kv_ref, None), (q_ref, qg_ref, qo_ref, SCALE)):
            a = ref[:, cols].astype(F32)
            a = a * lax.rsqrt(jnp.mean(a * a, axis=1, keepdims=True) + EPS) * gain[...]
            if scale is not None:
                a = a * scale
            out[0:rows, cols] = a.astype(BF)
    kv_ref[rows : rows + EXTRA, :] = f_ref[...]
    kv_ref[rows + EXTRA :, :] = v_ref[...]


def sums_row(extra, h, count):
    width = extra.shape[1]
    per = count // width
    parts = []
    for i in range(per):
        at = h * 3 * per + i
        parts.append(extra[at : at + 1] + extra[at + per : at + per + 1] + extra[at + 2 * per : at + 2 * per + 1])
    return jnp.concatenate(parts, axis=1)


def attend(own_ref, q_ref, k_ref, k_at, v_ref, v_at, m_ref, l_ref, a_ref, s_ref, p_ref, first):
    count = q_ref.shape[0]
    heads = q_ref.shape[1] // HEAD
    own = own_ref[...].astype(F32)
    extra = k_ref[k_at + count : k_at + count + EXTRA, :].astype(F32)
    part = 64
    ones = jnp.ones((count, HEAD), BF)
    biases = []
    for h in range(heads):
        cols = slice(h * HEAD, (h + 1) * HEAD)
        mine = sums_row(own, h, count)[:, count - 1 : count]
        biases.append((mine - sums_row(extra, h, count)) * LOG2E)
        s_ref[h] = lax.dot_general(
            q_ref[:, cols], k_ref[k_at : k_at + count, cols], (((1,), (1,)), ((), ())), preferred_element_type=F32
        )
    for h in range(heads):
        cols = slice(h * HEAD, (h + 1) * HEAD)

        def body(i, _):
            at = pl.ds(pl.multiple_of(i * part, part), part)
            s = s_ref[h, at, :] + biases[h]
            if first:
                row = i * part + lax.broadcasted_iota(jnp.int32, (part, count), 0)
                s = jnp.where(lax.broadcasted_iota(jnp.int32, (part, count), 1) <= row, s, -1e30)
                new = jnp.broadcast_to(jnp.max(s, axis=1, keepdims=True), (part, HEAD))
            else:
                old = m_ref[h, at, :]
                new = jnp.maximum(old, jnp.max(s, axis=1, keepdims=True))
                shrink = jnp.exp2(old - new)
                l_ref[h, at, :] = l_ref[h, at, :] * shrink
                a_ref[at, cols] = a_ref[at, cols] * shrink
            m_ref[h, at, :] = new
            p_ref[h, at, :] = jnp.exp2(s - new[:, 0:1]).astype(BF)
            return 0

        lax.fori_loop(0, count // part, body, 0, unroll=2)
        both = jnp.concatenate([v_ref[v_at : v_at + count, cols], ones], axis=1)
        got = jnp.dot(p_ref[h], both, preferred_element_type=F32)
        if first:
            a_ref[:, cols] = got[:, :HEAD]
            l_ref[h] = got[:, HEAD:]
        else:
            a_ref[:, cols] += got[:, :HEAD]
            l_ref[h] += got[:, HEAD:]


def self_kernel(own_ref, q_ref, kv_ref, m_ref, l_ref, a_ref, s_ref, p_ref):
    attend(own_ref, q_ref, kv_ref, 0, kv_ref, q_ref.shape[0] + EXTRA, m_ref, l_ref, a_ref, s_ref, p_ref, True)


def step_kernel(s, z_n, where, own_ref, q_ref, up, down, mi, li, ai, m_ref, l_ref, a_ref, s_ref, p_ref):
    m_ref[...] = mi[...]
    l_ref[...] = li[...]
    a_ref[...] = ai[...]
    z = where[0]
    for live, ref in ((z >= s, up), (z + s >= z_n, down)):

        @pl.when(live)
        def _(ref=ref):
            attend(own_ref, q_ref, ref, 0, ref, q_ref.shape[0] + EXTRA, m_ref, l_ref, a_ref, s_ref, p_ref, False)


def last_kernel(s, where, own_ref, q_ref, k_ref, v_ref, mi, li, ai, out_ref, m_ref, l_ref, a_ref, s_ref, p_ref):
    m_ref[...] = mi[...]
    l_ref[...] = li[...]
    a_ref[...] = ai[...]

    @pl.when(where[0] >= s)
    def _():
        attend(own_ref, q_ref, k_ref, 0, v_ref, 0, m_ref, l_ref, a_ref, s_ref, p_ref, False)

    for h in range(q_ref.shape[1] // HEAD):
        cols = slice(h * HEAD, (h + 1) * HEAD)
        out_ref[:, cols] = (a_ref[:, cols] / l_ref[h]).astype(BF)


def middle_kernel(places, where, *refs):
    n = len(places)
    att, res, wts = refs[0:n], refs[n : 2 * n], refs[2 * n : 3 * n]
    gain, normed_ref, own_ref, whole, mid = refs[3 * n :]
    rows, width = att[0].shape
    t = where[1]
    cols = []
    for by, flip in places:
        at = lax.rem(t + by, n)
        at = at + flip * (1 - 2 * lax.rem(at, 2))
        cols.append(pl.ds(pl.multiple_of(at * width, width), width))
    for i in range(n):
        whole[:, cols[i]] = att[i][...]
    for i in range(n):
        total = jnp.dot(whole[...], wts[i][...], preferred_element_type=F32) + res[i][...].astype(F32)
        total = total.astype(BF)
        mid[:, cols[i]] = total
        if i == 0:
            own_ref[...] = total
    part = rows // 8

    def norm(r, _):
        at = pl.ds(pl.multiple_of(r * part, part), part)
        w = mid[at, :].astype(F32)
        w = w * lax.rsqrt(jnp.mean(w * w, axis=1, keepdims=True) + EPS) * gain[...]
        normed_ref[at, :] = w.astype(BF)
        return 0

    lax.fori_loop(0, 8, norm, 0)


def hidden_kernel(places, z_n, where, *refs):
    n = len(places)
    a, b = refs[0:n], refs[n : 2 * n]
    normed, hid_ref, wa, wb = refs[2 * n :]
    z = where[0]
    for i, (by, row) in enumerate(places):
        count, depth = a[i].shape
        cols = pl.ds(pl.multiple_of(lax.rem(z + by + z_n, z_n) * depth, depth), depth)
        wa[row : row + count, cols] = a[i][...]
        wb[row : row + count, cols] = b[i][...]
    first = where[2] == 0
    x = normed[...]
    nt = (((1,), (1,)), ((), ()))
    u = lax.dot_general(x, wa[...], nt, preferred_element_type=F32)
    v = lax.dot_general(x, wb[...], nt, preferred_element_type=F32)
    gate = jnp.where(first, u, v)
    up = jnp.where(first, v, u)
    hid_ref[...] = (gate / (1.0 + jnp.exp(-gate)) * up).astype(BF)


def down_kernel(places, z_n, t_n, where, *refs):
    n = len(places)
    chunks, hid, outs, w = refs[0:n], refs[n], refs[n + 1 : n + 1 + t_n], refs[n + 1 + t_n]
    z, t = where[0], where[1]
    width = outs[0].shape[1]
    for i, (by, row) in enumerate(places):
        count, depth = chunks[i].shape
        block = lax.rem(z + by + z_n, z_n)
        per = width // depth
        owner = block // per
        chip = lax.rem(owner // 2 - t // 2 + t_n // 2, t_n // 2)
        apart = lax.rem(owner + t, 2)
        at = (apart * (t_n // 2) + chip) * width + lax.rem(block, per) * depth
        w[row : row + count, pl.ds(pl.multiple_of(at, depth), depth)] = chunks[i][...]
    x = hid[...]
    for i in range(t_n):
        outs[i][...] = jnp.dot(x, w[:, i * width : (i + 1) * width], preferred_element_type=F32).astype(BF)


PLACES = ((0, 0), (0, 1), (-2, 0), (-2, 1), (2, 0), (2, 1), (4, 0), (4, 1))


def together(*xs):
    return lax.optimization_barrier(xs)


def local(sizes, queries, key_vectors, value_vectors, forget_sums, residual, query_gain, key_gain, out_weight, norm_gain, gate_weight, up_weight, down_weight):
    g_n, z_n, t_n = sizes
    rows, width = queries.shape
    heads = width // HEAD
    half = rows // 2
    z, t, pair = lax.axis_index("sp"), lax.axis_index("tp"), lax.axis_index("grp") % 2
    where = jnp.stack([z, t, pair]).astype(jnp.int32)
    zu = lambda x: turn(x, "sp", z_n, 1)
    zd = lambda x: turn(x, "sp", z_n, -1)
    xu = lambda x: turn_x(x, t_n, 1)
    xd = lambda x: turn_x(x, t_n, -1)
    core = lambda x: swap_core(x, t_n)
    yy = lambda x: swap_pair(x, g_n)

    f = forget_sums.T
    f1 = lax.reduce_precision(f, 8, 7)
    f2 = lax.reduce_precision(f - f1, 8, 7)
    f3 = lax.reduce_precision(f - f1 - f2, 8, 7)
    terms = jnp.stack([f1, f2, f3], axis=1).reshape(-1, width)
    terms = jnp.pad(terms, ((0, EXTRA - terms.shape[0]), (0, 0))).astype(BF)

    sds = jax.ShapeDtypeStruct
    q, kv = call(
        prep_kernel, (sds((rows, width), BF), sds((2 * rows + EXTRA, width), BF)), [VMEM] * 6, "prep", 8
    )(queries, key_vectors, value_vectors, query_gain[None], key_gain[None], terms)

    state = (sds((heads, rows, HEAD), F32), sds((heads, rows, HEAD), F32), sds((rows, width), F32))
    tiles = [pltpu.VMEM((heads, rows, rows), F32), pltpu.VMEM((heads, rows, rows), BF)]

    gate_t, up_t, down_t = gate_weight.T, up_weight.T, down_weight.T
    own0 = jnp.where(pair == 0, gate_t, up_t)
    oth0 = jnp.where(pair == 0, up_t, gate_t)
    cut = (own0.shape[0] // 32) * 16 + (16 if own0.shape[0] % 32 else 0)

    own, oth, dn, places = [own0], [oth0], [down_t], [(0, 0)]
    far = z_n // 2
    ku = kd = kv
    gu = gd = own0
    du = dd = down_t
    start_down = far - 3
    st = None
    ys = ()
    res_l = res_r = wt_l = wt_r = None
    for s in range(1, far):
        if s > 1:
            ku, kd, *st = together(ku, kd, *st)
            if s == 3:
                ys += (res_l, res_r)
            if s == 4:
                ys += (wt_l, wt_r)
            if s == 5:
                ys += tuple(res[2:])
            if s == 7:
                ys += tuple(wts[2:6])
            gu, gd, *ys = together(gu, gd, *ys)
            ys = list(ys)
            if s == 3:
                res_l, res_r = ys[-2:]
            if s == 4:
                wt_l, wt_r = ys[-2:]
            if s == 5:
                res[2:] = ys[-6:]
                ys = ys[:-6]
            if s == 7:
                wts[2:6] = ys[-4:]
                ys = ys[:-4]
            if s >= 3:
                oth += ys[:2]
        nu, nd = zu(ku), zd(kd)
        hu, hd = zu(gu), zd(gd)
        if s >= start_down:
            if s > start_down:
                du, dd, nu, nd = together(du, dd, nu, nd)
            else:
                du, dd, ku = together(du, dd, ku)
            du, dd = zu(du), zd(dd)
            dn += [du, dd]
        if s == 1:
            res_l, res_r, wt_l, wt_r = xu(residual), xd(residual), xu(out_weight), xd(out_weight)
            res = [residual, core(residual)]
            wts = [out_weight, core(out_weight)]
            st = call(self_kernel, state, [VMEM] * 3, "attn_self", 16, tiles)(terms, q, kv)
            ys = ()
        else:
            ys = (yy(gu), yy(gd))
            st = call(functools.partial(step_kernel, s - 1, z_n), state, [SMEM] + [VMEM] * 7, "attn_step", 16, tiles)(
                where, terms, q, ku, kd, *st
            )
        if s == 3:
            fa, fb = xu(res_l[:half]), xd(res_r[half:])
            fr = jnp.concatenate([fa, fb], axis=0)
            res += [res_l, core(res_l), res_r, core(res_r), fr, core(fr)]
        if s == 4:
            wh = wt_l.shape[0] // 2
            fa, fb = xu(wt_l[:wh]), xd(wt_r[wh:])
            fw = jnp.concatenate([fa, fb], axis=0)
            wts += [wt_l, core(wt_l), wt_r, core(wt_r), fw]
        if s == 7:
            wts += [core(wts[6])]
        ku, kd, gu, gd = nu, nd, hu, hd
        own += [gu, gd]
        places += [(-s, 0), (s, 0)]

    ku, kd, *st = together(ku, kd, *st)
    gu, gd, *ys = together(gu, gd, *ys)
    oth += list(ys)
    kl, vl = zu(ku[: rows + EXTRA]), zd(kd[rows + EXTRA :])
    w1, w2 = zu(gu[:cut]), zd(gd[cut:])
    own += [w1, w2]
    places += [(far, 0), (far, cut)]
    y1, y2 = yy(gu), yy(gd)
    step_down = far - start_down
    du, dd, ku = together(du, dd, ku)
    du, dd = zu(du), zd(dd)
    dn += [du, dd]
    st = call(functools.partial(step_kernel, far - 1, z_n), state, [SMEM] + [VMEM] * 7, "attn_step", 16, tiles)(
        where, terms, q, ku, kd, *st
    )
    kl, vl, w1, w2, y1, y2, du, dd, *st = together(kl, vl, w1, w2, y1, y2, du, dd, *st)
    oth += [y1, y2]
    own[-2:] = [w1, w2]
    y3, y4 = yy(w1), yy(w2)
    oth += [y3, y4]
    du, dd = zu(du), zd(dd)
    dn += [du, dd]
    attended = call(
        functools.partial(last_kernel, far),
        sds((rows, width), BF),
        [SMEM] + [VMEM] * 7,
        "attn_last",
        16,
        [pltpu.VMEM(x.shape, x.dtype) for x in state] + tiles,
    )(where, terms, q, kl, vl, *st)

    attended, du, dd = together(attended, du, dd)
    left, right, other = xu(attended), xd(attended), core(attended)
    du, dd = zu(du), zd(dd)
    dn += [du, dd]
    left, right, du, dd = together(left, right, du, dd)
    fa, fb = xu(left[:half]), xd(right[half:])
    left_o, right_o = core(left), core(right)
    du, dd = zu(du), zd(dd)
    dn += [du, dd]
    fa, fb, du, dd = together(fa, fb, du, dd)
    fr = jnp.concatenate([fa, fb], axis=0)
    fr_o = core(fr)
    assert len(dn) == 2 * far - 1
    dn += [zu(du[:cut]), zd(dd[cut:])]
    att = [attended, other, left, left_o, right, right_o, fr, fr_o]
    d_model = width * t_n
    normed, mid_own = call(
        functools.partial(middle_kernel, PLACES_FOR(t_n)),
        (sds((rows, d_model), BF), sds((rows, width), BF)),
        [SMEM] + [VMEM] * (3 * t_n + 1),
        "middle",
        28,
        [pltpu.VMEM((rows, d_model), BF), pltpu.VMEM((rows, d_model), BF)],
    )(where, *att, *res, *wts, norm_gain[None])

    hid_w = own0.shape[0]
    n = len(places)
    hidden = call(
        functools.partial(hidden_kernel, places, z_n),
        sds((rows, hid_w), BF),
        [SMEM] + [VMEM] * (2 * n + 1),
        "hidden",
        28,
        [pltpu.VMEM((hid_w, d_model), BF)] * 2,
    )(where, *own, *oth, normed)

    k0, k1, k2, k3, a0, a1, a2, a3 = call(
        functools.partial(down_kernel, places, z_n, t_n),
        (sds((rows, width), BF),) * t_n,
        [SMEM] + [VMEM] * (n + 1),
        "down",
        20,
        [pltpu.VMEM((hid_w, d_model), BF)],
    )(where, *dn, hidden)

    r2, r1, r3, r0 = (core(a).astype(F32) for a in (a2, a1, a3, a0))
    far2 = k2.astype(F32) + r2
    s1 = k1.astype(F32) + r1
    s3 = k3.astype(F32) + r3
    f_up, f_dn = xu(far2[:half].astype(BF)), xd(far2[half:].astype(BF))
    e1, e3 = xu(s1[half:].astype(BF)), xd(s3[:half].astype(BF))
    g1 = xu((s1[:half] + f_up.astype(F32)).astype(BF))
    g3 = xd((s3[half:] + f_dn.astype(F32)).astype(BF))
    base = mid_own.astype(F32) + k0.astype(F32) + r0
    top = base[:half] + g1.astype(F32) + e3.astype(F32)
    low = base[half:] + e1.astype(F32) + g3.astype(F32)
    return jnp.concatenate([top, low], axis=0).astype(BF)


def PLACES_FOR(t_n):
    assert len(PLACES) == t_n
    return tuple((by % t_n, flip) for by, flip in PLACES)


def solution(mesh):
    sizes = (mesh.shape["grp"], mesh.shape["sp"], mesh.shape["tp"])
    rows = P(("grp", "sp"), "tp")
    placed = (rows,) * 5 + (P(), P(), P(None, "tp"), P()) + (P("sp", "tp"),) * 3
    return jax.shard_map(
        functools.partial(local, sizes), mesh=mesh, in_specs=placed, out_specs=rows, check_vma=False
    )
```
